32 devices in a mesh: sp: 8 (over z, core), tp: 4 (over y, x).
Axes of the slice: x: 2, y: 2, z: 4, core: 2. Of those that a mesh axis runs over, the one named last changes fastest.
Arguments:
- cell_query_heads: bfloat16 [1024, 2048], P('sp', 'tp'), may hold values from -6 to 6
- cell_key_heads: bfloat16 [1024, 2048], P('sp', 'tp'), may hold values from -6 to 6
- cell_value_heads: bfloat16 [1024, 2048], P('sp', 'tp'), may hold values from -6 to 6
- output_gate_logits: bfloat16 [1024, 2048], P('sp', 'tp'), may hold values from -6 to 6
- input_gate_log: float32 [1024, 16], P('sp', 'tp'), may hold values from -7 to 310
- forget_gate_logits: float32 [1024, 16], P('sp', 'tp'), may hold values from 1 to 14
- extra_log_decay: float32 [1024, 16], P('sp', 'tp'), may hold values from -1 to 0
- documents: int32 [1024], P('sp'), may hold values from 0 to 7, never falling along the last dimension, each value on 1 to 256 neighbouring positions
- head_norm_gain: float32 [2048], P('tp'), may hold values from 0.1 to 1.9
- stream: bfloat16 [1024, 4096], P('sp', 'tp'), may hold values from -6 to 6
- output_weight: bfloat16 [2048, 4096], P(None, 'tp'), may hold values from -0.125 to 0.125
- expert_norm_gain: bfloat16 [4096], P('tp'), may hold values from 0.099609375 to 1.8984375
- expert_choice_index: int32 [1024, 2], P('sp'), may hold values from 0 to 7, all different within a row; in each aligned block of 128 rows (0 to 127, 128 to 255, ...) at most 64 rows name the same one
- routing_weight: float32 [1024, 2], P('sp'), may hold values from 0.2 to 1
- gate_weight: bfloat16 [8, 4096, 2048], P('sp', None, 'tp'), may hold values from -0.09375 to 0.09375
- up_weight: bfloat16 [8, 4096, 2048], P('sp', None, 'tp'), may hold values from -0.09375 to 0.09375
- down_weight: bfloat16 [8, 2048, 4096], P('sp', None, 'tp'), may hold values from -0.125 to 0.125
Outputs:
- output: bfloat16 [1024, 4096], P('sp', 'tp')
The draws below stay inside these ranges and needn't reach their ends.
Inputs may be any that keep to these rules, and one draw needn't show every extreme that they name: `expert_choice_index`: in the rows of one index of sp no expert is named more than 64 times, a bound that some block reaches. `documents`: never falling; each document 1 to 256 positions, one exactly 256.
All inputs are finite; a program needn't handle non-finite values.
Results may differ from the reference program's by a relative error of at most 0.01.
Values may be sent and summed in bfloat16 or wider, within the bound.
A program may use at most 64 MiB of HBM per device.

```python
import math
import jax
import jax.numpy as jnp
import numpy as np
from jax import lax

D = 4096
CELL_HEADS = 16
HD = 128
FF = 2048
TOPK = 2
TOKENS_PER_SHARD = 128
DOCS = 8
SEQ = 1024
EXPERTS = 8
CAP = 64
DOC_MOST = 256
N_SP = 8


def draw_forget_gate_logits(key, part):
    head_key = jax.random.fold_in(key, 11)
    block_key = jax.random.fold_in(key, 12)
    noise_key = jax.random.fold_in(key, 13)
    fast_heads = jax.random.randint(head_key, (CELL_HEADS,), 0, 2) == 0
    level = jnp.where(fast_heads, jnp.log(40.0), jnp.log(SEQ / 1.5)).astype(jnp.float32)
    block_list = SEQ // TOKENS_PER_SHARD
    shift = jax.random.uniform(block_key, (block_list, 1, CELL_HEADS), jnp.float32, -0.7, 0.7)
    noise = 0.5 * jnp.clip(jax.random.normal(noise_key, (block_list, TOKENS_PER_SHARD, CELL_HEADS), jnp.float32), -3.0, 3.0)
    return (level[None, None, :] + shift + noise).reshape(SEQ, CELL_HEADS)


def draw_input_gate_log(key, part):
    base_key = jax.random.fold_in(key, 21)
    values = jnp.clip(jax.random.normal(base_key, (SEQ, CELL_HEADS), jnp.float32), -6.0, 6.0)
    return values


def draw_extra_log_decay(key, part):
    mark_key = jax.random.fold_in(key, 31)
    depth_key = jax.random.fold_in(key, 32)
    marks = jax.random.randint(mark_key, (SEQ, CELL_HEADS), 0, SEQ // 8) == 0
    depth = jax.random.uniform(depth_key, (SEQ, CELL_HEADS), jnp.float32, jnp.log(0.5), jnp.log(0.8))
    return jnp.where(marks, depth, 0.0).astype(jnp.float32)


def shard_levels(key, dims, pieces, smallest, high):
    level, own = 1.0, jax.random.fold_in(key, 6)
    for axis_at, parts in pieces:
        draws = jnp.exp(jax.random.uniform(jax.random.fold_in(own, axis_at), (parts,), jnp.float32, smallest / len(pieces), high / len(pieces)))
        level = level * jnp.repeat(draws, dims[axis_at] // parts).reshape([-1 if axis == axis_at else 1 for axis in range(len(dims))])
    return level


def length_profile(count, total, reach, slope):
    portions = [(1 << 20) // math.isqrt(rank ** slope) + 1 for rank in range(2, count + 1)]
    surplus, given = total - reach - (count - 1), [1] * (count - 1)
    while surplus > 0:
        free = [i for i in range(count - 1) if given[i] < reach]
        pool, left = sum([portions[i] for i in free]), surplus
        for i in free:
            extra = min(reach - given[i], max(1, left * portions[i] // pool), surplus)
            given[i] = given[i] + extra
            surplus = surplus - extra
    return np.array([reach] + given)


def ragged(own_key, number_of, total, limit, skew):
    if number_of == 2:
        one = jax.random.randint(own_key, (), max(1, total - limit), min(limit, total - 1) + 1)
        return jnp.stack([one, total - one])
    lengths = jnp.asarray(length_profile(number_of, total, limit, skew), jnp.int32)
    pairs = (number_of - 1) // 2
    giver, taker = lengths[1:1 + 2 * pairs:2], lengths[2:2 + 2 * pairs:2]
    margin = jnp.minimum(giver - 1, limit - taker)
    passed = jax.random.randint(jax.random.fold_in(own_key, 1), (pairs,), 0, 1 << 20) % (margin + 1)
    lengths = lengths.at[1:1 + 2 * pairs:2].set(giver - passed).at[2:2 + 2 * pairs:2].set(taker + passed)
    return lengths[jax.random.permutation(jax.random.fold_in(own_key, 2), number_of)]


def assign_block(stream_key, own, number, rows, number_of, top, most, lean):
    sequence = jax.random.permutation(stream_key, number_of)
    heavy_load, common = portions_of(number_of, rows * top, most, lean, True), portions_of(number_of, rows * top, most, lean, False)
    places = jnp.arange(number_of)

    def named(tallies, rotation):
        used = int((tallies > 0).sum())
        fixed = max(1, used // 4)
        moved = fixed + (places - fixed + rotation * (used - fixed)) % max(1, number_of - fixed)
        return jnp.zeros((number_of,), jnp.int32).at[sequence[jnp.where(places < fixed, places, moved)]].set(jnp.asarray(tallies, jnp.int32))

    tallies = jnp.where(number % 4 == 0, named(heavy_load, number // 4), named(common, number - number // 4 - 1))
    mixed = jax.random.permutation(jax.random.fold_in(own, 3), number_of)
    source_of, taker = mixed[0:number_of // 2 * 2:2], mixed[1:number_of // 2 * 2:2]
    room = jnp.minimum(tallies[source_of] - 1, most - tallies[taker]) // 2
    room = jnp.where((source_of == sequence[0]) | (taker == sequence[0]) | (tallies[taker] == 0), 0, jnp.maximum(room, 0))
    moved = jax.random.randint(jax.random.fold_in(own, 4), (number_of // 2,), 0, 1 << 20) % (room + 1)
    tallies = tallies.at[source_of].add(-moved).at[taker].add(moved)
    items = jnp.searchsorted(jnp.cumsum(tallies), jnp.arange(rows * top), side="right").astype(jnp.int32)
    table = items.reshape(top, rows).T
    table = table[jax.random.permutation(jax.random.fold_in(own, 1), rows)]
    rotation = jax.random.randint(jax.random.fold_in(own, 2), (rows, 1), 0, top)
    return jnp.take_along_axis(table, (jnp.arange(top)[None, :] + rotation) % top, axis=1)


def portions_of(number_of, total, most, skew, full):
    portions = [(1 << 20) // math.isqrt(rank ** skew) + 1 for rank in range(1, number_of + 1)]
    largest = most if full else min(most, max(-(-total // number_of), total * portions[0] // sum(portions)))
    least = 1 if total - largest >= number_of - 1 else 0
    given, rest = [largest] + [least] * (number_of - 1), total - largest - least * (number_of - 1)
    while rest > 0:
        free = [i for i in range(1, number_of) if given[i] < largest] or [i for i in range(1, number_of) if given[i] < most]
        pool, budget = sum([portions[i] for i in free]), rest
        for i in free:
            addition = min(most - given[i], max(1, budget * portions[i] // pool), rest)
            given[i] = given[i] + addition
            rest = rest - addition
    return np.array(given)


def centred(key, dims, scale, limit, split=(), held_as=jnp.bfloat16):
    drawn = jax.random.normal(key, dims, jnp.float32) * scale
    if len(split) > 0:
        drawn = shard_levels(key, dims, split, -0.22, 0.18) * drawn
    return jnp.clip(drawn, min=-limit, max=limit).astype(held_as)


def setup_inputs(seed: int = 0) -> dict:
    arg_keys = jax.random.split(jax.random.key(seed), 18)
    cell_query_heads = centred(arg_keys[0], (SEQ, CELL_HEADS * HD), 1.0, 6.0, ((0, 8), (1, 4)))
    cell_key_heads = centred(arg_keys[1], (SEQ, CELL_HEADS * HD), 1.0, 6.0, ((0, 8), (1, 4)))
    cell_value_heads = centred(arg_keys[2], (SEQ, CELL_HEADS * HD), 1.0, 6.0, ((0, 8), (1, 4)))
    output_gate_logits = centred(arg_keys[3], (SEQ, CELL_HEADS * HD), 1.0, 6.0, ((0, 8), (1, 4)))
    input_gate_log = draw_input_gate_log(jax.random.fold_in(arg_keys[17], 71), 0)
    forget_gate_logits = draw_forget_gate_logits(jax.random.fold_in(arg_keys[17], 71), 0)
    extra_log_decay = draw_extra_log_decay(jax.random.fold_in(arg_keys[17], 71), 0)
    documents = jnp.searchsorted(jnp.cumsum(ragged(arg_keys[7], DOCS, SEQ, DOC_MOST, 1)), jnp.arange(SEQ), side="right").astype(jnp.int32)
    head_norm_gain = jnp.clip(1.0 + 0.18 * jax.random.normal(arg_keys[8], (CELL_HEADS * HD,), jnp.float32), 0.1, 1.9)
    stream = centred(arg_keys[9], (SEQ, D), 1.0, 6.0, ((0, 8), (1, 4)))
    output_weight = centred(arg_keys[10], (CELL_HEADS * HD, D), (CELL_HEADS * HD) ** -0.5, 0.125, ((1, 4),))
    expert_norm_gain = jnp.clip(1.0 + 0.18 * jax.random.normal(arg_keys[11], (D,), jnp.float32), 0.099609375, 1.8984375).astype(jnp.bfloat16)
    expert_choice_index_keys = jax.random.split(jax.random.fold_in(arg_keys[12], 1), SEQ // TOKENS_PER_SHARD)
    expert_choice_index_turns = jax.random.permutation(jax.random.fold_in(arg_keys[12], 3), SEQ // TOKENS_PER_SHARD)
    expert_choice_index = jax.vmap(lambda own, number: assign_block(jax.random.fold_in(arg_keys[12], 2), own, number, TOKENS_PER_SHARD, EXPERTS, TOPK, CAP, 2))(expert_choice_index_keys, expert_choice_index_turns).reshape((SEQ, TOPK))
    routing_weight = jnp.clip(0.2 + 0.8 * jax.random.uniform(arg_keys[13], (SEQ, TOPK), jnp.float32) ** shard_levels(arg_keys[13], (SEQ, TOPK), ((0, 8),), -0.2, 0.2), 0.2, 1.0)
    gate_weight = centred(arg_keys[14], (EXPERTS, D, FF), D ** -0.5, 0.09375, ((0, 8), (2, 4)))
    up_weight = centred(arg_keys[15], (EXPERTS, D, FF), D ** -0.5, 0.09375, ((0, 8), (2, 4)))
    down_weight = centred(arg_keys[16], (EXPERTS, FF, D), FF ** -0.5, 0.125, ((0, 8), (2, 4)))
    return dict(cell_query_heads=cell_query_heads, cell_key_heads=cell_key_heads, cell_value_heads=cell_value_heads, output_gate_logits=output_gate_logits, input_gate_log=input_gate_log, forget_gate_logits=forget_gate_logits, extra_log_decay=extra_log_decay, documents=documents, head_norm_gain=head_norm_gain, stream=stream, output_weight=output_weight, expert_norm_gain=expert_norm_gain, expert_choice_index=expert_choice_index, routing_weight=routing_weight, gate_weight=gate_weight, up_weight=up_weight, down_weight=down_weight)


EPSILON = 1e-06
LOW_LOG = -1e+30
HIGHEST = lax.Precision.HIGHEST

def empty_summary(heads, width):
    return (jnp.zeros((heads, width, width), jnp.float32), jnp.zeros((heads, width), jnp.float32), jnp.full((heads,), LOW_LOG, jnp.float32), jnp.zeros((heads,), jnp.float32), jnp.zeros((), jnp.int32), jnp.full((), -1, jnp.int32), jnp.full((), -1, jnp.int32))

def block_summary(key_f, value_f, decay_logarithm, input_gate_log, documents, first_global):
    length = documents.shape[0]
    positions = jnp.arange(length, dtype=jnp.int32)
    cumulative = jnp.cumsum(decay_logarithm, axis=0)
    total_log = cumulative[-1]
    prior_log = cumulative - decay_logarithm
    starts = jnp.concatenate([jnp.reshape(first_global, (1,)), documents[1:] != documents[:-1]])
    inside = jnp.any(starts)
    last_start = jnp.max(jnp.where(starts, positions, -1))
    base_log = lax.optimization_barrier(jnp.sum(jnp.where((positions == last_start)[:, None], prior_log, 0.0), axis=0))
    in_last = (documents == documents[-1])[:, None]
    weight_log = total_log[None, :] - cumulative + input_gate_log
    peak_log = lax.optimization_barrier(jnp.max(jnp.where(in_last, weight_log, LOW_LOG), axis=0))
    peak_log = jnp.where(inside, jnp.maximum(peak_log, total_log - base_log), peak_log)
    weights = jnp.where(in_last, jnp.exp(jnp.minimum(weight_log - peak_log[None, :], 0.0)), 0.0)
    matrix = jnp.einsum('lhd,lhe->hde', weights[:, :, None] * key_f, value_f, precision=HIGHEST)
    normer = lax.optimization_barrier(jnp.sum(weights[:, :, None] * key_f, axis=0))
    return (matrix, normer, peak_log, total_log, inside.astype(jnp.int32), documents[0], documents[-1])

def combine(early, late):
    broken = late[5] != early[6]
    carry_matrix = jnp.where(broken, 0.0, early[0])
    carry_normer = jnp.where(broken, 0.0, early[1])
    carry_peak = jnp.where(broken, 0.0, early[2])
    joined = jnp.maximum(late[3] + carry_peak, late[2])
    older = jnp.exp(late[3] + carry_peak - joined)
    newer = jnp.exp(late[2] - joined)
    resets = late[4] > 0
    matrix = jnp.where(resets, late[0], older[:, None, None] * carry_matrix + newer[:, None, None] * late[0])
    normer = jnp.where(resets, late[1], older[:, None] * carry_normer + newer[:, None] * late[1])
    peak_log = jnp.where(resets, late[2], joined)
    flags = jnp.maximum(jnp.maximum(early[4], late[4]), broken.astype(jnp.int32))
    merged = (matrix, normer, peak_log, early[3] + late[3], flags, early[5], late[6])
    early_empty = early[6] < 0
    late_empty = late[6] < 0
    return tuple((jnp.where(early_empty, second, jnp.where(late_empty, first_item, joint)) for first_item, second, joint in zip(early, late, merged)))

def block_output(query_f, key_f, value_f, decay_logarithm, input_gate_log, documents, prefix):
    prev_matrix, prev_normer, prev_peak, _, _, _, prev_last = prefix
    length = documents.shape[0]
    positions = jnp.arange(length, dtype=jnp.int32)
    cumulative = jnp.cumsum(decay_logarithm, axis=0)
    prior_log = cumulative - decay_logarithm
    before = jnp.concatenate([jnp.reshape(prev_last, (1,)), documents[:-1]])
    starts = documents != before
    last_start = lax.cummax(jnp.where(starts, positions, -1), axis=0)
    started = last_start >= 0
    picker = (positions[None, :] == last_start[:, None]).astype(jnp.float32)
    base_log = jnp.dot(picker, prior_log, precision=HIGHEST)
    carry_log = (cumulative + jnp.where(started[:, None], -base_log, prev_peak[None, :])).T
    same_doc = (documents[:, None] == documents[None, :]) & (positions[:, None] >= positions[None, :])
    cum_heads = cumulative.T
    pair_log = cum_heads[:, :, None] - cum_heads[:, None, :] + input_gate_log.T[:, None, :]
    pair_log = jnp.where(same_doc[None], pair_log, LOW_LOG)
    peak_log = jnp.maximum(carry_log, lax.optimization_barrier(jnp.max(pair_log, axis=-1)))
    weights = jnp.exp(pair_log - peak_log[:, :, None])
    scores = jnp.einsum('lhd,shd->hls', query_f, key_f, precision=HIGHEST) * weights
    carry_scale = jnp.where(started[None, :], 0.0, jnp.exp(carry_log - peak_log))
    numer = jnp.einsum('hls,she->hle', scores, value_f, precision=HIGHEST)
    numer = numer + carry_scale[:, :, None] * jnp.einsum('lhd,hde->hle', query_f, prev_matrix, precision=HIGHEST)
    denom = lax.optimization_barrier(jnp.sum(scores, axis=-1)) + carry_scale * jnp.einsum('lhd,hd->hl', query_f, prev_normer, precision=HIGHEST)
    cell_vals = numer / jnp.maximum(jnp.abs(denom), jnp.exp(-peak_log))[:, :, None]
    return jnp.transpose(cell_vals, (1, 0, 2))

def finish_cell(cell_vals, output_gate_logits, head_norm_gain):
    length, heads, width = cell_vals.shape
    gated_cell = jax.nn.sigmoid(output_gate_logits.astype(jnp.float32)).reshape(length, heads, width) * cell_vals
    scaled = gated_cell * lax.rsqrt(lax.optimization_barrier(jnp.mean(gated_cell * gated_cell, axis=-1, keepdims=True)) + EPSILON)
    scaled = scaled * head_norm_gain.astype(jnp.float32).reshape(heads, width)
    return scaled.reshape(length, heads * width).astype(jnp.bfloat16)

def memory_cell_layer(cell_query_heads, cell_key_heads, cell_value_heads, output_gate_logits, input_gate_log, forget_gate_logits, extra_log_decay, documents, head_norm_gain):
    seq_len = documents.shape[0]
    block_list = seq_len // TOKENS_PER_SHARD
    shaped = (block_list, TOKENS_PER_SHARD, CELL_HEADS, HD)
    query_f = cell_query_heads.astype(jnp.float32).reshape(shaped)
    key_f = cell_key_heads.astype(jnp.float32).reshape(shaped) * HD ** (-0.5)
    value_f = cell_value_heads.astype(jnp.float32).reshape(shaped)
    decay_logarithm = (jax.nn.log_sigmoid(forget_gate_logits) + extra_log_decay).reshape(block_list, TOKENS_PER_SHARD, CELL_HEADS)
    gates = input_gate_log.reshape(block_list, TOKENS_PER_SHARD, CELL_HEADS)
    docs = documents.reshape(block_list, TOKENS_PER_SHARD)
    firsts = jnp.arange(block_list, dtype=jnp.int32) == 0
    summaries = lax.map(lambda items: block_summary(*items), (key_f, value_f, decay_logarithm, gates, docs, firsts))

    def advance(running, summary):
        return (combine(running, summary), running)
    _, prefixes = lax.scan(advance, empty_summary(CELL_HEADS, HD), summaries)
    cell_vals = lax.map(lambda items: block_output(*items), (query_f, key_f, value_f, decay_logarithm, gates, docs, prefixes))
    return finish_cell(cell_vals.reshape(seq_len, CELL_HEADS, HD), output_gate_logits, head_norm_gain)

def experts_layer(normed, expert_choice_index, routing_weight, gate_weight, up_weight, down_weight):
    seq_len = normed.shape[0]
    block_list = seq_len // TOKENS_PER_SHARD
    grouped = expert_choice_index.reshape(block_list, TOKENS_PER_SHARD * TOPK)
    onehot = (grouped[:, :, None] == jnp.arange(EXPERTS, dtype=jnp.int32)[None, None, :]).astype(jnp.int32)
    rank_in = lax.optimization_barrier(jnp.sum((jnp.cumsum(onehot, axis=1) - onehot) * onehot, axis=2))
    block_of = jnp.arange(block_list, dtype=jnp.int32)[:, None]
    slot_of = (grouped * (N_SP * CAP) + block_of * CAP + rank_in).reshape(-1).astype(jnp.int32)
    sources = jnp.repeat(normed, TOPK, axis=0)
    buffer = jnp.zeros((EXPERTS * N_SP * CAP, D), jnp.bfloat16).at[slot_of].set(sources)

    def run_expert(operands):
        row_block, gate_e, up_e, down_e = operands
        gate_act = jnp.dot(row_block, gate_e, preferred_element_type=jnp.float32)
        upward = jnp.dot(row_block, up_e, preferred_element_type=jnp.float32)
        hidden = (jax.nn.silu(gate_act) * upward).astype(jnp.bfloat16)
        return jnp.dot(hidden, down_e, preferred_element_type=jnp.float32).astype(jnp.bfloat16)
    served = lax.map(run_expert, (buffer.reshape(EXPERTS, N_SP * CAP, D), gate_weight, up_weight, down_weight))
    picked = served.reshape(-1, D)[slot_of].astype(jnp.float32).reshape(seq_len, TOPK, D)
    return lax.optimization_barrier(jnp.sum(picked * routing_weight[:, :, None], axis=1))

def reference(cell_query_heads, cell_key_heads, cell_value_heads, output_gate_logits, input_gate_log, forget_gate_logits, extra_log_decay, documents, head_norm_gain, stream, output_weight, expert_norm_gain, expert_choice_index, routing_weight, gate_weight, up_weight, down_weight):
    memory_cell_output = memory_cell_layer(cell_query_heads, cell_key_heads, cell_value_heads, output_gate_logits, input_gate_log, forget_gate_logits, extra_log_decay, documents, head_norm_gain)
    resid = (stream.astype(jnp.float32) + jnp.dot(memory_cell_output, output_weight, preferred_element_type=jnp.float32)).astype(jnp.bfloat16)
    rows_f = resid.astype(jnp.float32)
    normed = rows_f * lax.rsqrt(lax.optimization_barrier(jnp.mean(rows_f * rows_f, axis=1, keepdims=True)) + EPSILON)
    normed = (normed * expert_norm_gain.astype(jnp.float32)[None, :]).astype(jnp.bfloat16)
    mixed = experts_layer(normed, expert_choice_index, routing_weight, gate_weight, up_weight, down_weight)
    return (rows_f + mixed).astype(jnp.bfloat16)
```

```python
import functools

import jax
import jax.numpy as jnp
from jax import lax
from jax.experimental import pallas as pl
from jax.experimental.pallas import tpu as pltpu
from jax.sharding import PartitionSpec as P

D = 4096
HD = 128
TOPK = 2


EPSILON = 1e-06
LOW_LOG = -1e30
HIGHEST = lax.Precision.HIGHEST


def prefix_2(part, axis, combine, identity):
    place = lax.axis_index(axis)
    gathered = jax.tree.map(lambda a: lax.all_gather(a, axis), part)
    state = jax.tree.map(lambda a, e: jnp.zeros_like(a) + jnp.asarray(e, a.dtype), part, identity)

    def one(turn, state):
        return combine(
            state, jax.tree.map(lambda a: lax.dynamic_index_in_dim(a, turn, 0, False), gathered)
        )

    return lax.fori_loop(0, place, one, state)


def empty_summary(heads, width):
    return (
        jnp.zeros((heads, width, width), jnp.float32),
        jnp.zeros((heads, width), jnp.float32),
        jnp.full((heads,), LOW_LOG, jnp.float32),
        jnp.zeros((heads,), jnp.float32),
        jnp.zeros((), jnp.int32),
        jnp.full((), -1, jnp.int32),
        jnp.full((), -1, jnp.int32),
    )


def block_summary(key_f, value_f, decay_logarithm, input_gate_log, documents, first_global):
    length = documents.shape[0]
    positions = jnp.arange(length, dtype=jnp.int32)
    cumulative = jnp.cumsum(decay_logarithm, axis=0)
    total_log = cumulative[-1]
    prior_log = cumulative - decay_logarithm
    starts = jnp.concatenate([jnp.reshape(first_global, (1,)), documents[1:] != documents[:-1]])
    inside = jnp.any(starts)
    last_start = jnp.max(jnp.where(starts, positions, -1))
    base_log = jnp.sum(jnp.where((positions == last_start)[:, None], prior_log, 0.0), axis=0)
    in_last = (documents == documents[-1])[:, None]
    weight_log = total_log[None, :] - cumulative + input_gate_log
    peak_log = jnp.max(jnp.where(in_last, weight_log, LOW_LOG), axis=0)
    peak_log = jnp.where(inside, jnp.maximum(peak_log, total_log - base_log), peak_log)
    weights = jnp.where(in_last, jnp.exp(jnp.minimum(weight_log - peak_log[None, :], 0.0)), 0.0)
    matrix = jnp.einsum("lhd,lhe->hde", weights[:, :, None] * key_f, value_f, precision=HIGHEST)
    normer = jnp.sum(weights[:, :, None] * key_f, axis=0)
    return (
        matrix,
        normer,
        peak_log,
        total_log,
        inside.astype(jnp.int32),
        documents[0],
        documents[-1],
    )


def combine(early, late):
    broken = late[5] != early[6]
    carry_matrix = jnp.where(broken, 0.0, early[0])
    carry_normer = jnp.where(broken, 0.0, early[1])
    carry_peak = jnp.where(broken, 0.0, early[2])
    joined = jnp.maximum(late[3] + carry_peak, late[2])
    older = jnp.exp(late[3] + carry_peak - joined)
    newer = jnp.exp(late[2] - joined)
    resets = late[4] > 0
    matrix = jnp.where(
        resets, late[0], older[:, None, None] * carry_matrix + newer[:, None, None] * late[0]
    )
    normer = jnp.where(resets, late[1], older[:, None] * carry_normer + newer[:, None] * late[1])
    peak_log = jnp.where(resets, late[2], joined)
    flags = jnp.maximum(jnp.maximum(early[4], late[4]), broken.astype(jnp.int32))
    merged = (matrix, normer, peak_log, early[3] + late[3], flags, early[5], late[6])
    early_empty = early[6] < 0
    late_empty = late[6] < 0
    return tuple(
        (
            jnp.where(early_empty, second, jnp.where(late_empty, first_item, joint))
            for first_item, second, joint in zip(early, late, merged)
        )
    )


def block_output(query_f, key_f, value_f, decay_logarithm, input_gate_log, documents, prefix):
    prev_matrix, prev_normer, prev_peak, _, _, _, prev_last = prefix
    length = documents.shape[0]
    positions = jnp.arange(length, dtype=jnp.int32)
    cumulative = jnp.cumsum(decay_logarithm, axis=0)
    prior_log = cumulative - decay_logarithm
    before = jnp.concatenate([jnp.reshape(prev_last, (1,)), documents[:-1]])
    starts = documents != before
    last_start = lax.cummax(jnp.where(starts, positions, -1), axis=0)
    started = last_start >= 0
    picker = (positions[None, :] == last_start[:, None]).astype(jnp.float32)
    base_log = jnp.dot(picker, prior_log, precision=HIGHEST)
    carry_log = (cumulative + jnp.where(started[:, None], -base_log, prev_peak[None, :])).T
    same_doc = (documents[:, None] == documents[None, :]) & (
        positions[:, None] >= positions[None, :]
    )
    cum_heads = cumulative.T
    pair_log = cum_heads[:, :, None] - cum_heads[:, None, :] + input_gate_log.T[:, None, :]
    pair_log = jnp.where(same_doc[None], pair_log, LOW_LOG)
    peak_log = jnp.maximum(carry_log, jnp.max(pair_log, axis=-1))
    weights = jnp.exp(pair_log - peak_log[:, :, None])
    scores = jnp.einsum("lhd,shd->hls", query_f, key_f, precision=HIGHEST) * weights
    carry_scale = jnp.where(started[None, :], 0.0, jnp.exp(carry_log - peak_log))
    numer = jnp.einsum("hls,she->hle", scores, value_f, precision=HIGHEST)
    numer = numer + carry_scale[:, :, None] * jnp.einsum(
        "lhd,hde->hle", query_f, prev_matrix, precision=HIGHEST
    )
    denom = jnp.sum(scores, axis=-1) + carry_scale * jnp.einsum(
        "lhd,hd->hl", query_f, prev_normer, precision=HIGHEST
    )
    cell_vals = numer / jnp.maximum(jnp.abs(denom), jnp.exp(-peak_log))[:, :, None]
    return jnp.transpose(cell_vals, (1, 0, 2))


def finish_cell(cell_vals, output_gate_logits, head_norm_gain):
    length, heads, width = cell_vals.shape
    gated_cell = (
        jax.nn.sigmoid(output_gate_logits.astype(jnp.float32)).reshape(length, heads, width)
        * cell_vals
    )
    scaled = gated_cell * lax.rsqrt(
        jnp.mean(gated_cell * gated_cell, axis=-1, keepdims=True) + EPSILON
    )
    scaled = scaled * head_norm_gain.reshape(heads, width)
    return scaled.reshape(length, heads * width).astype(jnp.bfloat16)


MESH = pl.DeviceIdType.MESH
PARALLEL_LIMIT = 56 * 1024 * 1024


def remote(src, dst, send, recv, where):
    return pltpu.make_async_remote_copy(src, dst, send, recv, device_id=where, device_id_type=MESH)


def spread_own(teams, j, buf, row, height, width, chunk, send, recv):
    view = buf.at[pl.ds(row, height), pl.ds(pl.multiple_of(j * width, 128), width)]
    copies = []
    if teams == 4:
        for turn, peer in enumerate((j + 1 - 2 * lax.rem(j, 2), lax.rem(j + 2, 4))):
            copies.append(remote(view, view, send.at[chunk, turn], recv.at[chunk, turn], {"tp": peer}))
    else:
        for turn in range(teams - 1):
            peer = lax.rem(j + turn + 1, teams)
            copies.append(remote(view, view, send.at[chunk, turn], recv.at[chunk, turn], {"tp": peer}))
    return copies


def spread_relay(teams, j, buf, row, height, width, chunk, send, recv):
    if teams != 4:
        return []
    half = height // 2
    across, along = j + 1 - 2 * lax.rem(j, 2), lax.rem(j + 2, 4)
    first = buf.at[pl.ds(row, half), pl.ds(pl.multiple_of(across * width, 128), width)]
    second = buf.at[pl.ds(row + half, half), pl.ds(pl.multiple_of(along * width, 128), width)]
    return [
        remote(first, first, send.at[chunk, 2], recv.at[chunk, 2], {"tp": along}),
        remote(second, second, send.at[chunk, 3], recv.at[chunk, 3], {"tp": across}),
    ]


def expert_kernel(
    groups, teams, cap, each, chunks,
    normed, resid, chooser, selectors, weights, gate_hbm, up_hbm, down_hbm,
    out, packed, rows, hidden, result, returned, gate, up, down,
    load_sem, z_send, z_recv, t_send, t_recv, h_send, h_recv, r_send, r_recv,
):
    g, j = lax.axis_index("sp"), lax.axis_index("tp")
    own_chunk = g // each
    tall = each * cap
    width = normed.shape[1]
    hide = gate.shape[1]
    loads = [
        pltpu.make_async_copy(gate_hbm.at[0], gate, load_sem.at[0]),
        pltpu.make_async_copy(up_hbm.at[0], up, load_sem.at[1]),
        pltpu.make_async_copy(down_hbm.at[0], down, load_sem.at[2]),
    ]
    for load in loads:
        load.start()
    barrier = pltpu.get_barrier_semaphore()
    for step in range(1, groups):
        pl.semaphore_signal(
            barrier, inc=1, device_id={"sp": lax.rem(g + step, groups)}, device_id_type=MESH
        )
    if teams == 4:
        peers = (j + 1 - 2 * lax.rem(j, 2), lax.rem(j + 2, 4))
    else:
        peers = tuple(lax.rem(j + step, teams) for step in range(1, teams))
    for peer in peers:
        pl.semaphore_signal(barrier, inc=1, device_id={"tp": peer}, device_id_type=MESH)
    packed[...] = jnp.dot(chooser[...], normed[...], preferred_element_type=jnp.float32).astype(
        jnp.bfloat16
    )
    own = pl.ds(pl.multiple_of(g * cap, cap), cap)
    mine = pl.ds(pl.multiple_of(j * width, 128), width)
    rows[own, mine] = packed[own, :]
    pl.semaphore_wait(barrier, groups - 1 + len(peers))

    def dispatch(target):
        return remote(
            packed.at[pl.ds(pl.multiple_of(target * cap, cap), cap)],
            rows.at[own, mine],
            z_send.at[target],
            z_recv.at[g],
            {"sp": target},
        )

    def give_back(target):
        return remote(
            result.at[pl.ds(pl.multiple_of(target * cap, cap), cap)],
            returned.at[own],
            r_send.at[target],
            r_recv.at[g],
            {"sp": target},
        )

    def over_others(body):
        def one(turn, carry):
            target = lax.rem(own_chunk - turn // each + chunks, chunks) * each + lax.rem(turn, each)

            @pl.when(target != g)
            def _():
                body(target)

            return carry

        lax.fori_loop(0, groups, one, 0)

    over_others(lambda target: dispatch(target).start())

    def stage(i, carry):
        def chunk_of(k):
            return lax.rem(own_chunk + k, chunks)

        @pl.when(i < chunks)
        def _():
            c = chunk_of(i)
            row = pl.multiple_of(c * tall, tall)
            for p in range(each):
                source = c * each + p

                @pl.when(source != g)
                def _():
                    place = rows.at[pl.ds(pl.multiple_of(source * cap, cap), cap), mine]
                    remote(place, place, z_send.at[source], z_recv.at[source], {"sp": source}).wait_recv()

            for copy in spread_own(teams, j, rows, row, tall, width, c, t_send, t_recv):
                copy.start()

        @pl.when((i >= 1) & (i < chunks + 1))
        def _():
            c = chunk_of(i - 1)
            row = pl.multiple_of(c * tall, tall)
            for copy in spread_own(teams, j, rows, row, tall, width, c, t_send, t_recv):
                copy.wait_recv()
            for copy in spread_relay(teams, j, rows, row, tall, width, c, t_send, t_recv):
                copy.start()

        @pl.when((i >= 2) & (i < chunks + 2))
        def _():
            c = chunk_of(i - 2)
            row = pl.multiple_of(c * tall, tall)
            for copy in spread_relay(teams, j, rows, row, tall, width, c, t_send, t_recv):
                copy.wait_recv()

            @pl.when(i == 2)
            def _():
                for load in loads:
                    load.wait()

            block = rows[pl.ds(row, tall), :]
            opened = jnp.dot(block, gate[...], preferred_element_type=jnp.float32)
            raised = jnp.dot(block, up[...], preferred_element_type=jnp.float32)
            made = (opened * jax.nn.sigmoid(opened) * raised).astype(jnp.bfloat16)
            hidden[pl.ds(row, tall), pl.ds(pl.multiple_of(j * hide, 128), hide)] = made
            for copy in spread_own(teams, j, hidden, row, tall, hide, c, h_send, h_recv):
                copy.start()

        @pl.when((i >= 3) & (i < chunks + 3))
        def _():
            c = chunk_of(i - 3)
            row = pl.multiple_of(c * tall, tall)
            for copy in spread_own(teams, j, hidden, row, tall, hide, c, h_send, h_recv):
                copy.wait_recv()
            for copy in spread_relay(teams, j, hidden, row, tall, hide, c, h_send, h_recv):
                copy.start()

        @pl.when(i >= 4)
        def _():
            c = chunk_of(i - 4)
            row = pl.multiple_of(c * tall, tall)
            for copy in spread_relay(teams, j, hidden, row, tall, hide, c, h_send, h_recv):
                copy.wait_recv()
            result[pl.ds(row, tall), :] = jnp.dot(
                hidden[pl.ds(row, tall), :], down[...], preferred_element_type=jnp.float32
            ).astype(jnp.bfloat16)
            for p in range(each):
                target = c * each + p

                @pl.when(target != g)
                def _():
                    give_back(target).start()

                @pl.when(target == g)
                def _():
                    returned[own, :] = result[own, :]

        return carry

    lax.fori_loop(0, chunks + 4, stage, 0)

    def await_back(source):
        place = returned.at[pl.ds(pl.multiple_of(source * cap, cap), cap)]
        remote(place, place, r_send.at[source], r_recv.at[source], {"sp": source}).wait_recv()

    over_others(await_back)
    mixed = resid[...].astype(jnp.float32)
    for ordinal in range(TOPK):
        picked = jnp.dot(selectors[ordinal], returned[...], preferred_element_type=jnp.float32)
        mixed = mixed + weights[:, ordinal : ordinal + 1] * picked
    out[...] = mixed.astype(jnp.bfloat16)

    over_others(lambda target: dispatch(target).wait_send())
    over_others(lambda target: give_back(target).wait_send())

    def drain(c, carry):
        row = pl.multiple_of(c * tall, tall)
        for spread in (spread_own, spread_relay):
            for copy in spread(teams, j, rows, row, tall, width, c, t_send, t_recv):
                copy.wait_send()
            for copy in spread(teams, j, hidden, row, tall, hide, c, h_send, h_recv):
                copy.wait_send()
        return carry

    lax.fori_loop(0, chunks, drain, 0)


def experts(normed, resid, chooser, selectors, weights, gate_weight, up_weight, down_weight, cap):
    groups, teams = lax.axis_size("sp"), lax.axis_size("tp")
    slots = groups * cap
    each = max(1, min(groups, 128 // cap))
    chunks = groups // each
    tokens, width = normed.shape
    _, model, hide = gate_weight.shape
    _, hidden_all, _ = down_weight.shape
    ways = max(4, teams)
    vmem = pl.BlockSpec(memory_space=pltpu.VMEM)
    hbm = pl.BlockSpec(memory_space=pl.ANY)
    bf16 = jnp.bfloat16
    return pl.pallas_call(
        functools.partial(expert_kernel, groups, teams, cap, each, chunks),
        out_shape=jax.ShapeDtypeStruct((tokens, width), bf16),
        in_specs=[vmem] * 5 + [hbm] * 3,
        out_specs=vmem,
        scratch_shapes=[
            pltpu.VMEM((slots, width), bf16),
            pltpu.VMEM((slots, model), bf16),
            pltpu.VMEM((slots, hidden_all), bf16),
            pltpu.VMEM((slots, width), bf16),
            pltpu.VMEM((slots, width), bf16),
            pltpu.VMEM((model, hide), bf16),
            pltpu.VMEM((model, hide), bf16),
            pltpu.VMEM((hidden_all, width), bf16),
            pltpu.SemaphoreType.DMA((3,)),
            pltpu.SemaphoreType.DMA((groups,)),
            pltpu.SemaphoreType.DMA((groups,)),
            pltpu.SemaphoreType.DMA((chunks, ways)),
            pltpu.SemaphoreType.DMA((chunks, ways)),
            pltpu.SemaphoreType.DMA((chunks, ways)),
            pltpu.SemaphoreType.DMA((chunks, ways)),
            pltpu.SemaphoreType.DMA((groups,)),
            pltpu.SemaphoreType.DMA((groups,)),
        ],
        compiler_params=pltpu.CompilerParams(
            collective_id=1, has_side_effects=True, vmem_limit_bytes=PARALLEL_LIMIT
        ),
    )(normed, resid, chooser, selectors, weights, gate_weight, up_weight, down_weight)


def per_device(
    cell_query_heads,
    cell_key_heads,
    cell_value_heads,
    output_gate_logits,
    input_gate_log,
    forget_gate_logits,
    extra_log_decay,
    documents,
    head_norm_gain,
    stream,
    output_weight,
    expert_norm_gain,
    expert_choice_index,
    routing_weight,
    gate_weight,
    up_weight,
    down_weight,
):
    tokens = documents.shape[0]
    local_heads = input_gate_log.shape[1]
    shaped = (tokens, local_heads, HD)
    query_f = cell_query_heads.astype(jnp.float32).reshape(shaped)
    key_f = cell_key_heads.astype(jnp.float32).reshape(shaped) * HD ** (-0.5)
    value_f = cell_value_heads.astype(jnp.float32).reshape(shaped)
    decay_logarithm = jax.nn.log_sigmoid(forget_gate_logits) + extra_log_decay
    first_global = lax.axis_index("sp") == 0
    summary = block_summary(
        key_f, value_f, decay_logarithm, input_gate_log, documents, first_global
    )
    prefix = prefix_2(summary, "sp", combine, empty_summary(local_heads, HD))
    cell_vals = block_output(
        query_f, key_f, value_f, decay_logarithm, input_gate_log, documents, prefix
    )
    memory_cell_output = finish_cell(cell_vals, output_gate_logits, head_norm_gain)
    projected = jnp.dot(
        lax.all_gather(memory_cell_output, "tp", axis=1, tiled=True),
        output_weight,
        preferred_element_type=jnp.float32,
    )
    resid = (stream.astype(jnp.float32) + projected).astype(jnp.bfloat16)
    groups = lax.axis_size("sp")
    experts_all = groups * gate_weight.shape[0]
    capacity = 2 * tokens * TOPK // experts_all
    flat_ids = expert_choice_index.reshape(-1)
    onehot = (flat_ids[:, None] == jnp.arange(experts_all, dtype=jnp.int32)[None, :]).astype(
        jnp.int32
    )
    rank_in = jnp.sum((jnp.cumsum(onehot, axis=0) - onehot) * onehot, axis=1)
    slot_of = (flat_ids * capacity + rank_in).reshape(tokens, TOPK)
    slot_index = jnp.arange(experts_all * capacity, dtype=jnp.int32)
    chooser = jnp.any(slot_index[:, None, None] == slot_of[None, :, :], axis=2).astype(jnp.bfloat16)
    rows_f = resid.astype(jnp.float32)
    squares = lax.psum(jnp.sum(rows_f * rows_f, axis=1), "tp")
    normed = rows_f * lax.rsqrt(squares[:, None] / D + EPSILON)
    normed = (normed * expert_norm_gain.astype(jnp.float32)[None, :]).astype(jnp.bfloat16)
    selectors = (slot_of.T[:, :, None] == slot_index[None, None, :]).astype(jnp.bfloat16)
    return experts(
        normed, resid, chooser, selectors, routing_weight, gate_weight, up_weight, down_weight, capacity
    )


def solution(mesh):
    placed = (
        P("sp", "tp"),
        P("sp", "tp"),
        P("sp", "tp"),
        P("sp", "tp"),
        P("sp", "tp"),
        P("sp", "tp"),
        P("sp", "tp"),
        P("sp"),
        P("tp"),
        P("sp", "tp"),
        P(None, "tp"),
        P("tp"),
        P("sp", None),
        P("sp", None),
        P("sp", None, "tp"),
        P("sp", None, "tp"),
        P("sp", None, "tp"),
    )
    return jax.shard_map(
        per_device, mesh=mesh, in_specs=placed, out_specs=P("sp", "tp"), check_vma=False
    )
```
